512 devices in a mesh: ra: 64 (over z, y), cb: 8 (over x, core).
Axes of the slice: x: 4, y: 4, z: 16, core: 2. Of those that a mesh axis runs over, the one named last changes fastest.
Arguments:
- activations: bfloat16 [768, 4096], P('ra', 'cb'), may hold values from -230 to 230
- gain_first: float32 [4096], P('cb'), may hold values from 0.1 to 1.9
- gate_weight: float32 [11264, 4096], P('ra', 'cb'), may hold values from -0.25 to 0.25
- gate_scale: float32 [11264], P('ra'), may hold values from 0.5 to 2
- up_weight: float32 [11264, 4096], P('ra', 'cb'), may hold values from -0.25 to 0.25
- up_scale: float32 [11264], P('ra'), may hold values from 0.5 to 2
- down_weight: float32 [11264, 4096], P('ra', 'cb'), may hold values from -0.0546875 to 0.0546875
- down_scale: float32 [4096], P('cb'), may hold values from 0.35 to 2.8
- gain_second: float32 [4096], P('cb'), may hold values from 0.1 to 1.9
Outputs:
- normed: bfloat16 [768, 4096], P('ra', 'cb')
The draws below stay inside these ranges and needn't reach their ends.
All inputs are finite; a program needn't handle non-finite values.
Results may differ from the reference program's by a relative error of at most 0.011.
Values may be sent and summed in bfloat16 or wider, within the bound.
No kernel may reach another device: no remote copies, remote signals or barrier semaphores. Data moves between devices by JAX's collectives and lax.ppermute only.
A program may use at most 64 MiB of HBM per device.

```python
import math
import jax
import jax.numpy as jnp
from jax import lax

D = 4096
FF = 11264
TOKENS = 768


def draw_activations(key, part):
    first, second, third = jax.random.split(jax.random.fold_in(key, 17), 3)
    columns = jnp.arange(D, dtype=jnp.float32) / D
    column_factor = jnp.exp(jnp.log(4.0) * (columns - 0.5)) * jax.random.uniform(second, (D,), jnp.float32, 0.6, 1.4)
    base = jnp.clip(jax.random.normal(first, (TOKENS, D), jnp.float32), -5.0, 5.0)
    rows = jnp.exp(jax.random.uniform(third, (TOKENS, 1), jnp.float32, 0.0, jnp.log(10.0)))
    return (base * rows * column_factor).astype(jnp.bfloat16)


def draw_down_scale(key, part):
    columns = jnp.arange(D, dtype=jnp.float32) / D
    rising = jnp.exp(jnp.log(4.0) * (columns - 0.5))
    noise = jax.random.uniform(jax.random.fold_in(key, 29), (D,), jnp.float32, 0.7, 1.4)
    return rising * noise


def raised(drawn, stream_key, source, target, blocks, factor):
    owner, partner = [(jnp.arange(drawn.shape[position]) // (drawn.shape[position] // blocks)).reshape([-1 if axis == position else 1 for axis in range(drawn.ndim)]) for position in (source, target)]
    chosen = jax.random.permutation(stream_key, blocks)[partner]
    strong = (owner == chosen) | (owner == (partner + blocks // 2) % blocks)
    return jnp.where(strong, factor * drawn, drawn)


def block_levels(own_key, extent, pieces, low, largest):
    factor_of, own = 1.0, jax.random.fold_in(own_key, 6)
    for position, shards_of in pieces:
        draws = jnp.exp(jax.random.uniform(jax.random.fold_in(own, position), (shards_of,), jnp.float32, low / len(pieces), largest / len(pieces)))
        factor_of = factor_of * jnp.repeat(draws, extent[position] // shards_of).reshape([-1 if axis == position else 1 for axis in range(len(extent))])
    return factor_of


def centred(rng, extent, spread, reach, shards=(), held_as=jnp.bfloat16):
    entries = jax.random.normal(rng, extent, jnp.float32) * spread
    if len(shards) > 0:
        entries = block_levels(rng, extent, shards, -0.22, 0.18) * entries
    return jnp.clip(entries, min=-reach, max=reach).astype(held_as)


def bell_draw_with(rng, dims, width, most, cuts, heavy, kind=jnp.bfloat16):
    drawn = width * jax.random.normal(rng, dims, jnp.float32)
    if cuts:
        drawn = drawn * block_levels(rng, dims, cuts, -0.22, 0.18)
    return jnp.clip(raised(drawn, jax.random.fold_in(rng, 3), *heavy), -most, most).astype(kind)


def setup_inputs(seed: int = 0) -> dict:
    seeds = jax.random.split(jax.random.key(seed), 10)
    activations = draw_activations(jax.random.fold_in(seeds[9], 71), 0)
    gain_first = jnp.clip(1.0 + 0.18 * jax.random.normal(seeds[1], (D,), jnp.float32), 0.1, 1.9)
    gate_weight = bell_draw_with(seeds[2], (FF, D), D ** -0.5, 0.25, ((0, 64), (1, 8)), (1, 0, 64, 4.0), jnp.float32)
    gate_scale = jnp.clip(jnp.exp(math.log(2.0) - 1.3862944 * jax.random.uniform(seeds[3], (FF,), jnp.float32) ** block_levels(seeds[3], (FF,), ((0, 64),), -0.2, 0.2)), 0.5, 2.0)
    up_weight = bell_draw_with(seeds[4], (FF, D), D ** -0.5, 0.25, ((0, 64), (1, 8)), (1, 0, 64, 4.0), jnp.float32)
    up_scale = jnp.clip(jnp.exp(math.log(2.0) - 1.3862944 * jax.random.uniform(seeds[5], (FF,), jnp.float32) ** block_levels(seeds[5], (FF,), ((0, 64),), -0.2, 0.2)), 0.5, 2.0)
    down_weight = centred(seeds[6], (FF, D), FF ** -0.5, 0.0546875, ((0, 64), (1, 8)), jnp.float32)
    down_scale = draw_down_scale(jax.random.fold_in(seeds[9], 71), 0)
    gain_second = jnp.clip(1.0 + 0.18 * jax.random.normal(seeds[8], (D,), jnp.float32), 0.1, 1.9)
    return {"activations": activations, "gain_first": gain_first, "gate_weight": gate_weight, "gate_scale": gate_scale, "up_weight": up_weight, "up_scale": up_scale, "down_weight": down_weight, "down_scale": down_scale, "gain_second": gain_second}


EPS = 1e-06

def reference(activations, gain_first, gate_weight, gate_scale, up_weight, up_scale, down_weight, down_scale, gain_second):
    inputs = activations.astype(jnp.float32)
    rscale_first = lax.rsqrt(lax.optimization_barrier(jnp.mean(inputs * inputs, axis=1)) + EPS)[:, None]
    scaled = (inputs * gain_first).astype(jnp.bfloat16)
    gate_raw = jnp.dot(scaled, gate_weight.astype(jnp.bfloat16).T, preferred_element_type=jnp.float32)
    up_raw = jnp.dot(scaled, up_weight.astype(jnp.bfloat16).T, preferred_element_type=jnp.float32)
    gate = gate_raw * rscale_first * gate_scale
    up = up_raw * rscale_first * up_scale
    hidden = (jax.nn.silu(gate) * up).astype(jnp.bfloat16)
    mixed = jnp.dot(hidden, down_weight.astype(jnp.bfloat16), preferred_element_type=jnp.float32) * down_scale
    stream = 0.1 * inputs + mixed
    rscale_second = lax.rsqrt(lax.optimization_barrier(jnp.mean(stream * stream, axis=1)) + EPS)[:, None]
    return (stream * rscale_second * gain_second).astype(jnp.bfloat16)
```

```python
import jax
import jax.numpy as jnp
from jax import lax
from jax.sharding import Mesh
from jax.sharding import PartitionSpec as P

RA = ("zh", "zl", "y")
NEAR = ("zl", "y")
EPS = 1e-06


def from_everyone(value, axes):
    peers = lax.axis_size(axes)
    return lax.all_to_all(
        jnp.broadcast_to(value[None], (peers, *value.shape)), axes, 0, 0, tiled=True
    )


def gathered(value, axes):
    everything = from_everyone(value, axes)
    return everything.reshape(-1, *value.shape[1:])


def summed_on_arrival(value, axes):
    peers = lax.axis_size(axes)
    blocks = value.reshape(peers, -1, *value.shape[1:])
    arrived = lax.all_to_all(blocks, axes, 0, 0, tiled=True)
    return jnp.sum(arrived.astype(jnp.float32), axis=0)


def per_device(
    activations,
    gain_first,
    gate_weight,
    gate_scale,
    up_weight,
    up_scale,
    down_weight,
    down_scale,
    gain_second,
):
    bf16 = jnp.bfloat16
    units = gate_weight.shape[0]
    inputs = activations.astype(jnp.float32)
    features = activations.shape[1] * lax.axis_size("cb")
    both_local = jnp.concatenate([gate_weight, up_weight], axis=0).astype(bf16)
    down_local = down_weight.astype(bf16)

    tokens = gathered(gathered(activations, "zh"), NEAR)
    wide = tokens.astype(jnp.float32)
    squares = jnp.sum(wide * wide, axis=1, keepdims=True)
    squares_high = squares.astype(bf16)
    squares_low = (squares - squares_high.astype(jnp.float32)).astype(bf16)
    scaled = (wide * gain_first).astype(bf16)
    part = lax.dot_general(
        scaled, both_local, (((1,), (1,)), ((), ())), preferred_element_type=jnp.float32
    ).astype(bf16)
    full = summed_on_arrival(
        jnp.concatenate([part, squares_high, squares_low], axis=1), "cb"
    )
    total = full[:, 2 * units : 2 * units + 1] + full[:, 2 * units + 1 :]
    rscale_first = lax.rsqrt(total / features + EPS)
    gate = full[:, :units] * rscale_first * gate_scale
    up = full[:, units : 2 * units] * rscale_first * up_scale
    hidden = gathered((jax.nn.silu(gate) * up).astype(bf16), "cb")
    mixed = lax.dot_general(
        hidden, down_local, (((1,), (0,)), ((), ())), preferred_element_type=jnp.float32
    ).astype(bf16)
    near = summed_on_arrival(mixed, NEAR).astype(bf16)
    summed = summed_on_arrival(near, "zh")
    stream = 0.1 * inputs + summed * down_scale
    second = jnp.sum(from_everyone(jnp.sum(stream * stream, axis=1), "cb"), axis=0)
    rscale_second = lax.rsqrt(second / features + EPS)[:, None]
    return (stream * rscale_second * gain_second).astype(bf16)


def solution(mesh):
    torus = Mesh(
        mesh.devices.reshape(8, 2, 4, mesh.shape["cb"]), ("zh", "zl", "y", "cb")
    )
    in_specs = (
        P(RA, "cb"),
        P("cb"),
        P(RA, "cb"),
        P(RA),
        P(RA, "cb"),
        P(RA),
        P(RA, "cb"),
        P("cb"),
        P("cb"),
    )
    return jax.shard_map(
        per_device, mesh=torus, in_specs=in_specs, out_specs=P(RA, "cb"), check_vma=False
    )
```

```python
import jax
import jax.numpy as jnp
from jax import lax
from jax.sharding import Mesh
from jax.sharding import PartitionSpec as P


RA = ("z", "y")
EPS = 1e-06
PAD = 32


def from_everyone(value, axes):
    peers = lax.axis_size(axes)
    return lax.all_to_all(
        jnp.broadcast_to(value[None], (peers, *value.shape)), axes, 0, 0, tiled=True
    )


def gathered(value, axes):
    everything = from_everyone(value, axes)
    return everything.reshape(-1, *value.shape[1:])


def summed_on_arrival(value, axes):
    peers = lax.axis_size(axes)
    blocks = value.reshape(peers, -1, *value.shape[1:])
    arrived = lax.all_to_all(blocks, axes, 0, 0, tiled=True)
    return jnp.sum(arrived.astype(jnp.float32), axis=0)


def moved(value, axis, distance):
    size = lax.axis_size(axis)
    pairs = [(place, (place + distance) % size) for place in range(size)]
    return lax.ppermute(value, axis, pairs)


def in_three(value):
    terms = []
    for _ in range(3):
        term = lax.reduce_precision(value, 8, 7)
        terms.append(term.astype(jnp.bfloat16))
        value = value - term
    return terms


def per_device(
    activations,
    gain_first,
    gate_weight,
    gate_scale,
    up_weight,
    up_scale,
    down_weight,
    down_scale,
    gain_second,
):
    bf16, f32 = jnp.bfloat16, jnp.float32
    units, width = gate_weight.shape
    inputs = activations.astype(f32)
    features = width * lax.axis_size("cb")

    scales = jnp.stack(in_three(jnp.concatenate([gate_scale, up_scale])))
    scales = jnp.pad(scales, ((0, PAD // 2 - 3), (0, width - 2 * units)))
    own = jnp.concatenate(
        [
            gate_weight.astype(bf16),
            up_weight.astype(bf16),
            down_weight.astype(bf16),
            scales,
        ],
        axis=0,
    )
    half = own.shape[0] // 2
    before = moved(own, "y", 1)
    after = moved(own, "y", -1)
    upper = moved(before[:half], "y", 1)
    lower = moved(after[half:], "y", -1)
    column = [own, before, after, jnp.concatenate([upper, lower], axis=0)]

    tokens = gathered(activations, "z")
    wide = tokens.astype(f32)
    squares = jnp.sum(wide * wide, axis=1, keepdims=True)
    scaled = (wide * gain_first).astype(bf16)
    squares_high = lax.reduce_precision(squares, 8, 7)
    squares_low = lax.reduce_precision(squares - squares_high, 8, 7).astype(bf16)
    squares_high = squares_high.astype(bf16)
    filler = jnp.zeros((scaled.shape[0], PAD - 2), bf16)
    parts = []
    for block in column:
        part = lax.dot_general(
            scaled,
            block[: 2 * units],
            (((1,), (1,)), ((), ())),
            preferred_element_type=f32,
        )
        parts += [part.astype(bf16), squares_high, squares_low, filler]
    full = summed_on_arrival(jnp.concatenate(parts, axis=1), "cb")
    total = full[:, 2 * units] + full[:, 2 * units + 1]
    rscale_first = lax.rsqrt(total / features + EPS)[:, None]
    hidden = []
    for index, block in enumerate(column):
        scales = block[3 * units : 3 * units + 3, : 2 * units].astype(f32)
        scales = scales[0] + scales[1] + scales[2]
        first = index * (2 * units + PAD)
        gate = full[:, first : first + units] * rscale_first * scales[:units]
        first = first + units
        up = full[:, first : first + units] * rscale_first * scales[units:]
        hidden.append((jax.nn.silu(gate) * up).astype(bf16))
    hidden = gathered(jnp.concatenate(hidden, axis=1), "cb")
    down = jnp.concatenate([block[2 * units : 3 * units] for block in column], axis=0)
    mixed = lax.dot_general(
        hidden, down, (((1,), (0,)), ((), ())), preferred_element_type=f32
    ).astype(bf16)
    summed = summed_on_arrival(mixed, "z")
    stream = 0.1 * inputs + summed * down_scale
    second = jnp.sum(from_everyone(jnp.sum(stream * stream, axis=1), "cb"), axis=0)
    rscale_second = lax.rsqrt(second / features + EPS)[:, None]
    return (stream * rscale_second * gain_second).astype(bf16)


def solution(mesh):
    torus = Mesh(mesh.devices.reshape(16, 4, mesh.shape["cb"]), ("z", "y", "cb"))
    in_specs = (
        P(RA, "cb"),
        P("cb"),
        P(RA, "cb"),
        P(RA),
        P(RA, "cb"),
        P(RA),
        P(RA, "cb"),
        P("cb"),
        P("cb"),
    )
    return jax.shard_map(
        per_device, mesh=torus, in_specs=in_specs, out_specs=P(RA, "cb"), check_vma=False
    )
```

```python
import jax
import jax.numpy as jnp
from jax import lax
from jax.experimental import pallas as pl
from jax.experimental.pallas import tpu as pltpu
from jax.sharding import Mesh
from jax.sharding import PartitionSpec as P


RA = ("z", "y")
EPS = 1e-06
LANES = 128
WIDE = 384
SPLIT = 256


def whole(value):
    shape = value.shape
    return pl.BlockSpec(shape, lambda _: (0,) * len(shape))


def local(kernel, out, args, specs=None, **cost):
    return pl.pallas_call(
        kernel,
        grid=(1,),
        in_specs=specs or [whole(arg) for arg in args],
        out_specs=whole(out),
        out_shape=out,
        compiler_params=pltpu.CompilerParams(vmem_limit_bytes=16 * 2**20),
        cost_estimate=pl.CostEstimate(
            flops=cost.get("flops", 10**6),
            bytes_accessed=sum(arg.size * arg.dtype.itemsize for arg in (*args, out)),
            transcendentals=0,
        ),
    )(*args)


def pack_kernel(
    gate_hbm,
    up_hbm,
    down_hbm,
    gate_scale_hbm,
    up_scale_hbm,
    gain_first_hbm,
    gain_second_hbm,
    down_scale_hbm,
    out_ref,
    gain_first_ref,
    gain_second_ref,
    down_scale_ref,
    gate_ref,
    up_ref,
    down_ref,
    gate_scale_ref,
    up_scale_ref,
    end_ref,
    sems,
):
    bf16, f32 = jnp.bfloat16, jnp.float32
    units = gate_ref.shape[0]
    rest = units - LANES
    pairs = (
        (gate_hbm, gate_ref),
        (up_hbm, up_ref),
        (gate_scale_hbm, gate_scale_ref),
        (up_scale_hbm, up_scale_ref),
        (down_hbm, down_ref),
        (gain_first_hbm, gain_first_ref),
        (gain_second_hbm, gain_second_ref),
        (down_scale_hbm, down_scale_ref),
    )
    copies = [
        pltpu.make_async_copy(source, target, sems.at[place])
        for place, (source, target) in enumerate(pairs)
    ]
    for copy in copies:
        copy.start()
    end_ref[...] = jnp.zeros_like(end_ref)

    second = 2 * LANES
    third = second + rest
    fourth = third + rest
    copies[0].wait()
    out_ref[0:LANES] = gate_ref[0:LANES].astype(bf16)
    out_ref[second:third] = gate_ref[LANES:units].astype(bf16)
    copies[1].wait()
    out_ref[LANES:second] = up_ref[0:LANES].astype(bf16)
    out_ref[third:fourth] = up_ref[LANES:units].astype(bf16)

    copies[2].wait()
    copies[3].wait()
    end_ref[0:1, 0:rest] = gate_scale_ref[0:1, LANES:units]
    end_ref[8:9, 0:rest] = up_scale_ref[0:1, LANES:units]
    ends = end_ref[0:8] + pltpu.roll(end_ref[8:16], rest, 1)
    tiles = (gate_scale_ref[0:1, 0:LANES], up_scale_ref[0:1, 0:LANES], ends[0:1])
    row = lax.broadcasted_iota(jnp.int32, (WIDE - fourth, LANES), 0)
    for place, value in enumerate(tiles):
        high = value.astype(bf16).astype(f32)
        left = value - high
        middle = left.astype(bf16).astype(f32)
        low = left - middle
        pad = jnp.where(row == 0, high, 0.0)
        pad = jnp.where(row == 1, middle, pad)
        pad = jnp.where(row == 2, low, pad)
        out_ref[fourth:WIDE, place * LANES : (place + 1) * LANES] = pad.astype(bf16)
    out_ref[fourth:WIDE, 3 * LANES :] = jnp.zeros(
        (WIDE - fourth, out_ref.shape[1] - 3 * LANES), bf16
    )
    copies[4].wait()
    out_ref[WIDE : WIDE + units] = down_ref[...].astype(bf16)
    for copy in copies[5:]:
        copy.wait()


def part_kernel(
    token_ref, gain_ref, own_ref, before_ref, after_ref, upper_ref, lower_ref, out_ref
):
    bf16, f32 = jnp.bfloat16, jnp.float32
    wide = token_ref[...].astype(f32)
    squares = jnp.sum(wide * wide, axis=1, keepdims=True)
    high = squares.astype(bf16).astype(f32)
    low = squares - high
    scaled = (wide * gain_ref[...]).astype(bf16)

    def product(rows):
        return lax.dot_general(
            scaled, rows, (((1,), (1,)), ((), ())), preferred_element_type=f32
        )

    used = WIDE - 32
    first = product(own_ref[0:WIDE])
    place = lax.broadcasted_iota(jnp.int32, first.shape, 1)
    first = jnp.where(place == used, high, first)
    first = jnp.where(place == used + 1, low, first)
    out_ref[:, 0:WIDE] = first.astype(bf16)
    out_ref[:, WIDE : 2 * WIDE] = product(before_ref[0:WIDE]).astype(bf16)
    out_ref[:, 2 * WIDE : 3 * WIDE] = product(after_ref[0:WIDE]).astype(bf16)
    last = 3 * WIDE + SPLIT
    out_ref[:, 3 * WIDE : last] = product(upper_ref[...]).astype(bf16)
    out_ref[:, last : 4 * WIDE] = product(lower_ref[0 : WIDE - SPLIT]).astype(bf16)


def hidden_kernel(
    features, rest, part_ref, own_ref, before_ref, after_ref, lower_ref, out_ref
):
    bf16, f32 = jnp.bfloat16, jnp.float32
    peers, _, _ = out_ref.shape
    used = WIDE - 32

    def summed(first):
        total = part_ref[0, :, first : first + LANES].astype(f32)
        for peer in range(1, peers):
            total = total + part_ref[peer, :, first : first + LANES].astype(f32)
        return total

    mixed = summed(2 * LANES)
    place = lax.broadcasted_iota(jnp.int32, mixed.shape, 1)
    mark = used - 2 * LANES
    squares = jnp.where((place == mark) | (place == mark + 1), mixed, 0.0)
    squares = jnp.sum(squares, axis=1, keepdims=True)
    rscale = lax.rsqrt(squares / features + EPS)

    def store(first, value):
        for peer in range(peers):
            out_ref[peer, :, first : first + LANES] = value.astype(bf16)

    def gated(gate, up):
        return gate / (1.0 + jnp.exp(-gate)) * up

    ends = []
    for index, ref in enumerate((own_ref, before_ref, after_ref, lower_ref)):
        scales = ref[...].astype(f32)
        scales = scales[0:1] + scales[1:2] + scales[2:3]
        first = index * WIDE
        gate = summed(first) * rscale * scales[:, 0:LANES]
        up = summed(first + LANES) * rscale * scales[:, LANES : 2 * LANES]
        store(index * LANES, gated(gate, up))
        end = mixed if index == 0 else summed(first + 2 * LANES)
        end = end * rscale * scales[:, 2 * LANES : 3 * LANES]
        end = gated(end, pltpu.roll(end, LANES - rest, 1))
        ends.append(jnp.where(place < rest, end, 0.0))
    for pair in range(2):
        joined = ends[2 * pair] + pltpu.roll(ends[2 * pair + 1], LANES // 2, 1)
        store((4 + pair) * LANES, joined)


def down_kernel(
    rest, hidden_ref, own_ref, before_ref, after_ref, lower_ref, out_ref, ends_ref
):
    f32 = jnp.float32
    total = None
    ends_ref[...] = jnp.zeros_like(ends_ref)
    for index, ref in enumerate((own_ref, before_ref, after_ref, lower_ref)):
        first = WIDE - SPLIT if index == 3 else WIDE
        value = jnp.dot(
            hidden_ref[:, index * LANES : (index + 1) * LANES],
            ref[first : first + LANES],
            preferred_element_type=f32,
        )
        total = value if total is None else total + value
        start = index * (LANES // 2)
        ends_ref[start : start + rest] = ref[first + LANES : first + LANES + rest]
    total = total + jnp.dot(
        hidden_ref[:, 4 * LANES : 6 * LANES], ends_ref[...], preferred_element_type=f32
    )
    out_ref[...] = total.astype(out_ref.dtype)


def from_everyone(value, axes):
    peers = lax.axis_size(axes)
    return lax.all_to_all(
        jnp.broadcast_to(value[None], (peers, *value.shape)), axes, 0, 0, tiled=True
    )


def moved(value, axis, distance):
    size = lax.axis_size(axis)
    pairs = [(place, (place + distance) % size) for place in range(size)]
    return lax.ppermute(value, axis, pairs)


def per_device(
    activations,
    gain_first,
    gate_weight,
    gate_scale,
    up_weight,
    up_scale,
    down_weight,
    down_scale,
    gain_second,
):
    bf16, f32 = jnp.bfloat16, jnp.float32
    units, width = gate_weight.shape
    rest = units - LANES
    peers = lax.axis_size("cb")
    features = width * peers
    shape = jax.ShapeDtypeStruct

    inputs = activations.astype(f32)
    weight, scale, vector = (units, width), (1, units), pltpu.VMEM((1, width), f32)
    outs = (pltpu.VMEM((WIDE + units, width), bf16), vector, vector, vector)
    own, gain_first, gain_second, down_scale = pl.pallas_call(
        pack_kernel,
        in_specs=[pl.BlockSpec(memory_space=pltpu.MemorySpace.HBM)] * 8,
        out_specs=[pl.BlockSpec(memory_space=pltpu.MemorySpace.VMEM)] * 4,
        out_shape=outs,
        scratch_shapes=[
            *[pltpu.VMEM(weight, f32)] * 3,
            *[pltpu.VMEM(scale, f32)] * 2,
            pltpu.VMEM((16, LANES), f32),
            pltpu.SemaphoreType.DMA((8,)),
        ],
        compiler_params=pltpu.CompilerParams(vmem_limit_bytes=65000000),
        cost_estimate=pl.CostEstimate(
            flops=10**6, bytes_accessed=2**20, transcendentals=0
        ),
    )(
        gate_weight,
        up_weight,
        down_weight,
        gate_scale[None],
        up_scale[None],
        gain_first[None],
        gain_second[None],
        down_scale[None],
    )
    before = moved(own, "y", 1)
    after = moved(own, "y", -1)
    upper = moved(before[:SPLIT], "y", 1)
    lower = moved(after[SPLIT:], "y", -1)

    rows = activations.reshape(-1, 4, width)
    tokens = from_everyone(rows, "z")
    tokens = tokens.reshape(-1, width)
    count = tokens.shape[0]
    part = local(
        part_kernel,
        shape((count, 4 * WIDE), bf16),
        (tokens, gain_first, own, before, after, upper, lower),
        flops=2 * count * width * 4 * WIDE,
    )
    part = lax.all_to_all(part.reshape(peers, -1, 4 * WIDE), "cb", 0, 0, tiled=True)

    def scale_rows(first):
        return pl.BlockSpec((16, width), lambda _: (first // 16, 0))

    args = (part, own, before, after, lower)
    hidden = local(
        lambda *refs: hidden_kernel(features, rest, *refs),
        shape((peers, count // peers, 6 * LANES), bf16),
        args,
        specs=[whole(part)]
        + [scale_rows(2 * units)] * 3
        + [scale_rows(2 * units - SPLIT)],
    )
    hidden = lax.all_to_all(hidden, "cb", 0, 0, tiled=True).reshape(count, 6 * LANES)
    args = (hidden, own, before, after, lower)
    out = shape((count, width), bf16)
    mixed = pl.pallas_call(
        lambda *refs: down_kernel(rest, *refs),
        grid=(1,),
        in_specs=[whole(arg) for arg in args],
        out_specs=whole(out),
        out_shape=out,
        scratch_shapes=[pltpu.VMEM((2 * LANES, width), bf16)],
        compiler_params=pltpu.CompilerParams(vmem_limit_bytes=16 * 2**20),
        cost_estimate=pl.CostEstimate(
            flops=2 * count * width * 6 * LANES, bytes_accessed=2**20, transcendentals=0
        ),
    )(*args)
    blocks = mixed.reshape(lax.axis_size("z"), -1, 4, width)
    summed = lax.all_to_all(blocks, "z", 0, 0, tiled=True)
    summed = jnp.sum(summed.astype(f32), axis=0).reshape(-1, width)
    stream = 0.1 * inputs + summed * down_scale
    second = jnp.sum(from_everyone(jnp.sum(stream * stream, axis=1), "cb"), axis=0)
    rscale_second = lax.rsqrt(second / features + EPS)[:, None]
    return (stream * rscale_second * gain_second).astype(bf16)


def solution(mesh):
    torus = Mesh(mesh.devices.reshape(16, 4, mesh.shape["cb"]), ("z", "y", "cb"))
    in_specs = (
        P(RA, "cb"),
        P("cb"),
        P(RA, "cb"),
        P(RA),
        P(RA, "cb"),
        P(RA),
        P(RA, "cb"),
        P("cb"),
        P("cb"),
    )
    return jax.shard_map(
        per_device, mesh=torus, in_specs=in_specs, out_specs=P(RA, "cb"), check_vma=False
    )
```

```python
import jax
import jax.numpy as jnp
from jax import lax
from jax.experimental import pallas as pl
from jax.experimental.pallas import tpu as pltpu
from jax.sharding import Mesh
from jax.sharding import PartitionSpec as P


RA = ("z", "y")
EPS = 1e-06
LANES = 128
USED = 352
DOWN = 368
WIDE = 384
SPLIT = 224


def whole(value):
    shape = value.shape
    return pl.BlockSpec(shape, lambda _: (0,) * len(shape))


def local(kernel, out, args, specs=None, scratch=(), flops=10**6):
    return pl.pallas_call(
        kernel,
        grid=(1,),
        in_specs=specs or [whole(arg) for arg in args],
        out_specs=whole(out),
        out_shape=out,
        scratch_shapes=scratch,
        compiler_params=pltpu.CompilerParams(vmem_limit_bytes=16 * 2**20),
        cost_estimate=pl.CostEstimate(
            flops=flops,
            bytes_accessed=sum(arg.size * arg.dtype.itemsize for arg in (*args, out)),
            transcendentals=0,
        ),
    )(*args)


def pack_kernel(
    gate_hbm,
    up_hbm,
    down_hbm,
    gate_scale_hbm,
    up_scale_hbm,
    gain_first_hbm,
    gain_second_hbm,
    down_scale_hbm,
    rows_hbm,
    out_ref,
    gain_first_ref,
    gain_second_ref,
    down_scale_ref,
    rows_ref,
    sent_hbm,
    gate_ref,
    up_ref,
    down_ref,
    gate_scale_ref,
    up_scale_ref,
    end_ref,
    block_ref,
    sems,
):
    bf16, f32 = jnp.bfloat16, jnp.float32
    units = gate_ref.shape[0]
    rest = units - LANES
    pairs = (
        (rows_hbm, rows_ref),
        (gate_hbm, gate_ref),
        (up_hbm, up_ref),
        (gate_scale_hbm, gate_scale_ref),
        (up_scale_hbm, up_scale_ref),
        (down_hbm, down_ref),
        (gain_first_hbm, gain_first_ref),
        (gain_second_hbm, gain_second_ref),
        (down_scale_hbm, down_scale_ref),
    )
    copies = [
        pltpu.make_async_copy(source, target, sems.at[place])
        for place, (source, target) in enumerate(pairs)
    ]
    for copy in copies:
        copy.start()
    end_ref[...] = jnp.zeros_like(end_ref)

    second = 2 * LANES
    third = second + rest
    fourth = third + rest
    copies[0].wait()
    rows = rows_ref[...].astype(f32)
    blocks, size, _ = block_ref.shape
    for block in range(blocks):
        block_ref[block] = rows[block * size : (block + 1) * size].astype(bf16)
    sends = [
        pltpu.make_async_copy(block_ref, sent_hbm.at[peer], sems.at[len(copies) + peer])
        for peer in range(sent_hbm.shape[0])
    ]
    for send in sends:
        send.start()
    copies[1].wait()
    out_ref[0:LANES] = gate_ref[0:LANES].astype(bf16)
    out_ref[second:third] = gate_ref[LANES:units].astype(bf16)
    copies[2].wait()
    out_ref[LANES:second] = up_ref[0:LANES].astype(bf16)
    out_ref[third:fourth] = up_ref[LANES:units].astype(bf16)

    copies[3].wait()
    copies[4].wait()
    end_ref[0:1, 0:rest] = gate_scale_ref[0:1, LANES:units]
    end_ref[8:9, 0:rest] = up_scale_ref[0:1, LANES:units]
    ends = end_ref[0:8] + pltpu.roll(end_ref[8:16], rest, 1)
    tiles = (gate_scale_ref[0:1, 0:LANES], up_scale_ref[0:1, 0:LANES], ends[0:1])
    row = lax.broadcasted_iota(jnp.int32, (DOWN - fourth, LANES), 0)
    for place, value in enumerate(tiles):
        high = value.astype(bf16).astype(f32)
        left = value - high
        middle = left.astype(bf16).astype(f32)
        low = left - middle
        pad = jnp.where(row == 0, high, 0.0)
        pad = jnp.where(row == 1, middle, pad)
        pad = jnp.where(row == 2, low, pad)
        out_ref[fourth:DOWN, place * LANES : (place + 1) * LANES] = pad.astype(bf16)
    out_ref[fourth:DOWN, 3 * LANES :] = jnp.zeros(
        (DOWN - fourth, out_ref.shape[1] - 3 * LANES), bf16
    )
    copies[5].wait()
    out_ref[DOWN : DOWN + units] = down_ref[...].astype(bf16)
    for copy in copies[6:] + sends:
        copy.wait()


def part_kernel(
    token_ref,
    gain_ref,
    own_ref,
    before_ref,
    after_ref,
    upper_ref,
    lower_ref,
    out_ref,
    far_ref,
):
    bf16, f32 = jnp.bfloat16, jnp.float32
    wide = token_ref[...].astype(f32)
    squares = jnp.sum(wide * wide, axis=1, keepdims=True)
    high = squares.astype(bf16).astype(f32)
    low = squares - high
    scaled = (wide * gain_ref[...]).astype(bf16)

    def product(rows):
        return lax.dot_general(
            scaled, rows, (((1,), (1,)), ((), ())), preferred_element_type=f32
        )

    far_ref[0:SPLIT] = upper_ref[...]
    far_ref[SPLIT:WIDE] = lower_ref[0 : WIDE - SPLIT]
    first = product(own_ref[0:WIDE])
    place = lax.broadcasted_iota(jnp.int32, first.shape, 1)
    first = jnp.where(place == USED, high, first)
    first = jnp.where(place == USED + 1, low, first)
    out_ref[:, 0:WIDE] = first.astype(bf16)
    out_ref[:, WIDE : 2 * WIDE] = product(before_ref[0:WIDE]).astype(bf16)
    out_ref[:, 2 * WIDE : 3 * WIDE] = product(after_ref[0:WIDE]).astype(bf16)
    out_ref[:, 3 * WIDE : 4 * WIDE] = product(far_ref[...]).astype(bf16)


def hidden_kernel(
    features, rest, part_ref, own_ref, before_ref, after_ref, lower_ref, out_ref
):
    bf16, f32 = jnp.bfloat16, jnp.float32
    peers, _, _ = out_ref.shape

    def summed(first):
        total = part_ref[0, :, first : first + LANES].astype(f32)
        for peer in range(1, peers):
            total = total + part_ref[peer, :, first : first + LANES].astype(f32)
        return total

    mixed = summed(2 * LANES)
    place = lax.broadcasted_iota(jnp.int32, mixed.shape, 1)
    mark = USED - 2 * LANES
    squares = jnp.where((place == mark) | (place == mark + 1), mixed, 0.0)
    squares = jnp.sum(squares, axis=1, keepdims=True)
    rscale = lax.rsqrt(squares / features + EPS)

    def store(first, value):
        for peer in range(peers):
            out_ref[peer, :, first : first + LANES] = value.astype(bf16)

    def gated(gate, up):
        return gate / (1.0 + jnp.exp(-gate)) * up

    ends = []
    for index, ref in enumerate((own_ref, before_ref, after_ref, lower_ref)):
        scales = ref[...].astype(f32)
        scales = scales[0:1] + scales[1:2] + scales[2:3]
        first = index * WIDE
        gate = summed(first) * rscale * scales[:, 0:LANES]
        up = summed(first + LANES) * rscale * scales[:, LANES : 2 * LANES]
        store(index * LANES, gated(gate, up))
        end = mixed if index == 0 else summed(first + 2 * LANES)
        end = end * rscale * scales[:, 2 * LANES : 3 * LANES]
        end = gated(end, pltpu.roll(end, LANES - rest, 1))
        ends.append(jnp.where(place < rest, end, 0.0))
    for pair in range(2):
        joined = ends[2 * pair] + pltpu.roll(ends[2 * pair + 1], LANES // 2, 1)
        store((4 + pair) * LANES, joined)


def down_kernel(
    rest, hidden_ref, own_ref, before_ref, after_ref, lower_ref, out_ref, ends_ref
):
    f32 = jnp.float32
    total = None
    ends_ref[...] = jnp.zeros_like(ends_ref)
    for index, ref in enumerate((own_ref, before_ref, after_ref, lower_ref)):
        first = DOWN - SPLIT if index == 3 else DOWN
        value = jnp.dot(
            hidden_ref[:, index * LANES : (index + 1) * LANES],
            ref[first : first + LANES],
            preferred_element_type=f32,
        )
        total = value if total is None else total + value
        start = index * (LANES // 2)
        ends_ref[start : start + rest] = ref[first + LANES : first + LANES + rest]
    total = total + jnp.dot(
        hidden_ref[:, 4 * LANES : 6 * LANES], ends_ref[...], preferred_element_type=f32
    )
    out_ref[...] = total.astype(out_ref.dtype)


def from_everyone(value, axes):
    peers = lax.axis_size(axes)
    return lax.all_to_all(
        jnp.broadcast_to(value[None], (peers, *value.shape)), axes, 0, 0, tiled=True
    )


def moved(value, axis, distance):
    size = lax.axis_size(axis)
    pairs = [(place, (place + distance) % size) for place in range(size)]
    return lax.ppermute(value, axis, pairs)


def per_device(
    activations,
    gain_first,
    gate_weight,
    gate_scale,
    up_weight,
    up_scale,
    down_weight,
    down_scale,
    gain_second,
):
    bf16, f32 = jnp.bfloat16, jnp.float32
    units, width = gate_weight.shape
    rest = units - LANES
    peers = lax.axis_size("cb")
    features = width * peers
    shape = jax.ShapeDtypeStruct

    weight, scale, vector = (units, width), (1, units), pltpu.VMEM((1, width), f32)
    columns = lax.axis_size("z")
    block = (activations.shape[0] // 4, 4, width)
    sent = shape((columns, *block), bf16)
    own = pltpu.VMEM((DOWN + units, width), bf16)
    rows = pltpu.VMEM(activations.shape, bf16)
    outs = (own, vector, vector, vector, rows, sent)
    own, gain_first, gain_second, down_scale, rows, sent = pl.pallas_call(
        pack_kernel,
        in_specs=[pl.BlockSpec(memory_space=pltpu.MemorySpace.HBM)] * 9,
        out_specs=[pl.BlockSpec(memory_space=pltpu.MemorySpace.VMEM)] * 5
        + [pl.BlockSpec(memory_space=pltpu.MemorySpace.HBM)],
        out_shape=outs,
        scratch_shapes=[
            *[pltpu.VMEM(weight, f32)] * 3,
            *[pltpu.VMEM(scale, f32)] * 2,
            pltpu.VMEM((16, LANES), f32),
            pltpu.VMEM(block, bf16),
            pltpu.SemaphoreType.DMA((9 + columns,)),
        ],
        compiler_params=pltpu.CompilerParams(vmem_limit_bytes=65000000),
        cost_estimate=pl.CostEstimate(
            flops=10**6, bytes_accessed=2**20, transcendentals=0
        ),
    )(
        gate_weight,
        up_weight,
        down_weight,
        gate_scale[None],
        up_scale[None],
        gain_first[None],
        gain_second[None],
        down_scale[None],
        activations,
    )
    before = moved(own, "y", 1)
    after = moved(own, "y", -1)
    upper = moved(before[:SPLIT], "y", 1)
    lower = moved(after[SPLIT:], "y", -1)

    tokens = lax.all_to_all(sent, "z", 0, 0, tiled=True)
    tokens = tokens.reshape(-1, width)
    count = tokens.shape[0]
    part = local(
        part_kernel,
        shape((count, 4 * WIDE), bf16),
        (tokens, gain_first, own, before, after, upper, lower),
        scratch=[pltpu.VMEM((WIDE, width), bf16)],
        flops=2 * count * width * 4 * WIDE,
    )
    part = lax.all_to_all(part.reshape(peers, -1, 4 * WIDE), "cb", 0, 0, tiled=True)

    def scale_rows(first):
        return pl.BlockSpec((16, width), lambda _: (first // 16, 0))

    args = (part, own, before, after, lower)
    hidden = local(
        lambda *refs: hidden_kernel(features, rest, *refs),
        shape((peers, count // peers, 6 * LANES), bf16),
        args,
        specs=[whole(part)]
        + [scale_rows(2 * units)] * 3
        + [scale_rows(2 * units - SPLIT)],
    )
    hidden = lax.all_to_all(hidden, "cb", 0, 0, tiled=True).reshape(count, 6 * LANES)
    mixed = local(
        lambda *refs: down_kernel(rest, *refs),
        shape((count, width), bf16),
        (hidden, own, before, after, lower),
        scratch=[pltpu.VMEM((2 * LANES, width), bf16)],
        flops=2 * count * width * 6 * LANES,
    )
    blocks = mixed.reshape(columns, -1, 4, width)
    summed = lax.all_to_all(blocks, "z", 0, 0, tiled=True)
    summed = jnp.sum(summed.astype(f32), axis=0).reshape(-1, width)
    stream = 0.1 * rows.astype(f32) + summed * down_scale
    second = jnp.sum(from_everyone(jnp.sum(stream * stream, axis=1), "cb"), axis=0)
    rscale_second = lax.rsqrt(second / features + EPS)[:, None]
    return (stream * rscale_second * gain_second).astype(bf16)


def solution(mesh):
    torus = Mesh(mesh.devices.reshape(16, 4, mesh.shape["cb"]), ("z", "y", "cb"))
    in_specs = (
        P(RA, "cb"),
        P("cb"),
        P(RA, "cb"),
        P(RA),
        P(RA, "cb"),
        P(RA),
        P(RA, "cb"),
        P("cb"),
        P("cb"),
    )
    return jax.shard_map(
        per_device, mesh=torus, in_specs=in_specs, out_specs=P(RA, "cb"), check_vma=False
    )
```

```python
import jax
import jax.numpy as jnp
from jax import lax
from jax.experimental import pallas as pl
from jax.experimental.pallas import tpu as pltpu
from jax.sharding import Mesh
from jax.sharding import PartitionSpec as P


RA = ("z", "y")
EPS = 1e-06
GATHER = [[*range(10, 16), *range(10)]]
SUM = [[*range(10, 16), *range(10)]]
NEAR = [[*range(5, 8), *range(5)]]
LANES = 128
USED = 352
DOWN = 368
WIDE = 384
SPLIT = 160


def whole(value):
    shape = value.shape
    return pl.BlockSpec(shape, lambda _: (0,) * len(shape))


def local(kernel, out, args, specs=None, scratch=(), flops=10**6):
    return pl.pallas_call(
        kernel,
        grid=(1,),
        in_specs=specs or [whole(arg) for arg in args],
        out_specs=whole(out),
        out_shape=out,
        scratch_shapes=scratch,
        compiler_params=pltpu.CompilerParams(vmem_limit_bytes=16 * 2**20),
        cost_estimate=pl.CostEstimate(
            flops=flops,
            bytes_accessed=sum(arg.size * arg.dtype.itemsize for arg in (*args, out)),
            transcendentals=0,
        ),
    )(*args)


def pack_kernel(
    gate_hbm,
    up_hbm,
    down_hbm,
    gate_scale_hbm,
    up_scale_hbm,
    gain_first_hbm,
    gain_second_hbm,
    down_scale_hbm,
    rows_hbm,
    out_ref,
    gain_first_ref,
    gain_second_ref,
    down_scale_ref,
    rows_ref,
    sent_hbm,
    gate_ref,
    up_ref,
    down_ref,
    gate_scale_ref,
    up_scale_ref,
    end_ref,
    block_ref,
    sems,
):
    bf16, f32 = jnp.bfloat16, jnp.float32
    units = gate_ref.shape[0]
    rest = units - LANES
    pairs = (
        (rows_hbm, rows_ref),
        (gate_hbm, gate_ref),
        (up_hbm, up_ref),
        (gate_scale_hbm, gate_scale_ref),
        (up_scale_hbm, up_scale_ref),
        (down_hbm, down_ref),
        (gain_first_hbm, gain_first_ref),
        (gain_second_hbm, gain_second_ref),
        (down_scale_hbm, down_scale_ref),
    )
    copies = [
        pltpu.make_async_copy(source, target, sems.at[place])
        for place, (source, target) in enumerate(pairs)
    ]
    for copy in copies:
        copy.start()
    end_ref[...] = jnp.zeros_like(end_ref)

    second = 2 * LANES
    third = second + rest
    fourth = third + rest
    copies[0].wait()
    rows = rows_ref[...].astype(f32)
    blocks, size, _ = block_ref.shape
    for block in range(blocks):
        block_ref[block] = rows[block * size : (block + 1) * size].astype(bf16)
    sends = [
        pltpu.make_async_copy(block_ref, sent_hbm.at[peer], sems.at[len(copies) + peer])
        for peer in range(sent_hbm.shape[0])
    ]
    for send in sends:
        send.start()
    copies[1].wait()
    out_ref[0:LANES] = gate_ref[0:LANES].astype(bf16)
    out_ref[second:third] = gate_ref[LANES:units].astype(bf16)
    copies[2].wait()
    out_ref[LANES:second] = up_ref[0:LANES].astype(bf16)
    out_ref[third:fourth] = up_ref[LANES:units].astype(bf16)

    copies[3].wait()
    copies[4].wait()
    end_ref[0:1, 0:rest] = gate_scale_ref[0:1, LANES:units]
    end_ref[8:9, 0:rest] = up_scale_ref[0:1, LANES:units]
    ends = end_ref[0:8] + pltpu.roll(end_ref[8:16], rest, 1)
    tiles = (gate_scale_ref[0:1, 0:LANES], up_scale_ref[0:1, 0:LANES], ends[0:1])
    row = lax.broadcasted_iota(jnp.int32, (DOWN - fourth, LANES), 0)
    for place, value in enumerate(tiles):
        high = value.astype(bf16).astype(f32)
        left = value - high
        middle = left.astype(bf16).astype(f32)
        low = left - middle
        pad = jnp.where(row == 0, high, 0.0)
        pad = jnp.where(row == 1, middle, pad)
        pad = jnp.where(row == 2, low, pad)
        out_ref[fourth:DOWN, place * LANES : (place + 1) * LANES] = pad.astype(bf16)
    out_ref[fourth:DOWN, 3 * LANES :] = jnp.zeros(
        (DOWN - fourth, out_ref.shape[1] - 3 * LANES), bf16
    )
    copies[5].wait()
    out_ref[DOWN : DOWN + units] = down_ref[...].astype(bf16)
    for copy in copies[6:] + sends:
        copy.wait()


def part_kernel(
    token_ref,
    gain_ref,
    own_ref,
    before_ref,
    after_ref,
    upper_ref,
    lower_ref,
    out_ref,
    far_ref,
):
    bf16, f32 = jnp.bfloat16, jnp.float32
    wide = token_ref[...].astype(f32)
    squares = jnp.sum(wide * wide, axis=1, keepdims=True)
    high = squares.astype(bf16).astype(f32)
    low = squares - high
    scaled = (wide * gain_ref[...]).astype(bf16)

    def product(rows):
        return lax.dot_general(
            scaled, rows, (((1,), (1,)), ((), ())), preferred_element_type=f32
        )

    far_ref[0:SPLIT] = upper_ref[...]
    far_ref[SPLIT:WIDE] = lower_ref[0 : WIDE - SPLIT]
    first = product(own_ref[0:WIDE])
    place = lax.broadcasted_iota(jnp.int32, first.shape, 1)
    first = jnp.where(place == USED, high, first)
    first = jnp.where(place == USED + 1, low, first)
    out_ref[:, 0:WIDE] = first.astype(bf16)
    out_ref[:, WIDE : 2 * WIDE] = product(before_ref[0:WIDE]).astype(bf16)
    out_ref[:, 2 * WIDE : 3 * WIDE] = product(after_ref[0:WIDE]).astype(bf16)
    out_ref[:, 3 * WIDE : 4 * WIDE] = product(far_ref[...]).astype(bf16)


def hidden_kernel(
    features, rest, part_ref, own_ref, before_ref, after_ref, lower_ref, out_ref
):
    bf16, f32 = jnp.bfloat16, jnp.float32
    peers, _, _ = out_ref.shape

    def summed(first):
        total = part_ref[0, :, first : first + LANES].astype(f32)
        for peer in range(1, peers):
            total = total + part_ref[peer, :, first : first + LANES].astype(f32)
        return total

    mixed = summed(2 * LANES)
    place = lax.broadcasted_iota(jnp.int32, mixed.shape, 1)
    mark = USED - 2 * LANES
    squares = jnp.where((place == mark) | (place == mark + 1), mixed, 0.0)
    squares = jnp.sum(squares, axis=1, keepdims=True)
    rscale = lax.rsqrt(squares / features + EPS)

    def store(first, value):
        for peer in range(peers):
            out_ref[peer, :, first : first + LANES] = value.astype(bf16)

    def gated(gate, up):
        return gate / (1.0 + jnp.exp(-gate)) * up

    ends = []
    for index, ref in enumerate((own_ref, before_ref, after_ref, lower_ref)):
        scales = ref[...].astype(f32)
        scales = scales[0:1] + scales[1:2] + scales[2:3]
        first = index * WIDE
        gate = summed(first) * rscale * scales[:, 0:LANES]
        up = summed(first + LANES) * rscale * scales[:, LANES : 2 * LANES]
        store(index * LANES, gated(gate, up))
        end = mixed if index == 0 else summed(first + 2 * LANES)
        end = end * rscale * scales[:, 2 * LANES : 3 * LANES]
        end = gated(end, pltpu.roll(end, LANES - rest, 1))
        ends.append(jnp.where(place < rest, end, 0.0))
    for pair in range(2):
        joined = ends[2 * pair] + pltpu.roll(ends[2 * pair + 1], LANES // 2, 1)
        store((4 + pair) * LANES, joined)


def down_kernel(
    rest, hidden_ref, own_ref, before_ref, after_ref, lower_ref, out_ref, ends_ref
):
    f32 = jnp.float32
    total = None
    ends_ref[...] = jnp.zeros_like(ends_ref)
    for index, ref in enumerate((own_ref, before_ref, after_ref, lower_ref)):
        first = DOWN - SPLIT if index == 3 else DOWN
        value = jnp.dot(
            hidden_ref[:, index * LANES : (index + 1) * LANES],
            ref[first : first + LANES],
            preferred_element_type=f32,
        )
        total = value if total is None else total + value
        start = index * (LANES // 2)
        ends_ref[start : start + rest] = ref[first + LANES : first + LANES + rest]
    total = total + jnp.dot(
        hidden_ref[:, 4 * LANES : 6 * LANES], ends_ref[...], preferred_element_type=f32
    )
    out_ref[...] = total.astype(out_ref.dtype)


def moved(value, axis, distance):
    size = lax.axis_size(axis)
    pairs = [(place, (place + distance) % size) for place in range(size)]
    return lax.ppermute(value, axis, pairs)


def per_device(
    activations,
    gain_first,
    gate_weight,
    gate_scale,
    up_weight,
    up_scale,
    down_weight,
    down_scale,
    gain_second,
):
    bf16, f32 = jnp.bfloat16, jnp.float32
    units, width = gate_weight.shape
    rest = units - LANES
    peers = lax.axis_size("cb")
    features = width * peers
    shape = jax.ShapeDtypeStruct

    weight, scale, vector = (units, width), (1, units), pltpu.VMEM((1, width), f32)
    columns = lax.axis_size("z")
    block = (activations.shape[0] // 4, 4, width)
    sent = shape((columns, *block), bf16)
    own = pltpu.VMEM((DOWN + units, width), bf16)
    rows = pltpu.VMEM(activations.shape, bf16)
    outs = (own, vector, vector, vector, rows, sent)
    own, gain_first, gain_second, down_scale, rows, sent = pl.pallas_call(
        pack_kernel,
        in_specs=[pl.BlockSpec(memory_space=pltpu.MemorySpace.HBM)] * 9,
        out_specs=[pl.BlockSpec(memory_space=pltpu.MemorySpace.VMEM)] * 5
        + [pl.BlockSpec(memory_space=pltpu.MemorySpace.HBM)],
        out_shape=outs,
        scratch_shapes=[
            *[pltpu.VMEM(weight, f32)] * 3,
            *[pltpu.VMEM(scale, f32)] * 2,
            pltpu.VMEM((16, LANES), f32),
            pltpu.VMEM(block, bf16),
            pltpu.SemaphoreType.DMA((9 + columns,)),
        ],
        compiler_params=pltpu.CompilerParams(vmem_limit_bytes=65000000),
        cost_estimate=pl.CostEstimate(
            flops=10**6, bytes_accessed=2**20, transcendentals=0
        ),
    )(
        gate_weight,
        up_weight,
        down_weight,
        gate_scale[None],
        up_scale[None],
        gain_first[None],
        gain_second[None],
        down_scale[None],
        activations,
    )
    before = moved(own, "y", 1)
    after = moved(own, "y", -1)
    upper = moved(before[:SPLIT], "y", 1)
    lower = moved(after[SPLIT:], "y", -1)

    tokens = lax.all_to_all(sent, "z", 0, 0, tiled=True, axis_index_groups=GATHER)
    tokens = tokens.reshape(-1, width)
    count = tokens.shape[0]
    part = local(
        part_kernel,
        shape((count, 4 * WIDE), bf16),
        (tokens, gain_first, own, before, after, upper, lower),
        scratch=[pltpu.VMEM((WIDE, width), bf16)],
        flops=2 * count * width * 4 * WIDE,
    )
    part = part.reshape(peers, -1, 4 * WIDE)
    part = lax.all_to_all(part, "cb", 0, 0, tiled=True, axis_index_groups=NEAR)

    def scale_rows(first):
        return pl.BlockSpec((16, width), lambda _: (first // 16, 0))

    args = (part, own, before, after, lower)
    hidden = local(
        lambda *refs: hidden_kernel(features, rest, *refs),
        shape((peers, count // peers, 6 * LANES), bf16),
        args,
        specs=[whole(part)]
        + [scale_rows(2 * units)] * 3
        + [scale_rows(2 * units - SPLIT)],
    )
    hidden = lax.all_to_all(hidden, "cb", 0, 0, tiled=True, axis_index_groups=NEAR)
    hidden = hidden.reshape(count, 6 * LANES)
    mixed = local(
        lambda *refs: down_kernel(rest, *refs),
        shape((count, width), bf16),
        (hidden, own, before, after, lower),
        scratch=[pltpu.VMEM((2 * LANES, width), bf16)],
        flops=2 * count * width * 6 * LANES,
    )
    blocks = mixed.reshape(columns, -1, 4, width)
    summed = lax.all_to_all(blocks, "z", 0, 0, tiled=True, axis_index_groups=SUM)
    summed = jnp.sum(summed.astype(f32), axis=0).reshape(-1, width)
    stream = 0.1 * rows.astype(f32) + summed * down_scale
    second = jnp.sum(stream * stream, axis=1)
    second = jnp.broadcast_to(second, (peers, *second.shape))
    second = lax.all_to_all(second, "cb", 0, 0, tiled=True, axis_index_groups=NEAR)
    second = jnp.sum(second, axis=0)
    rscale_second = lax.rsqrt(second / features + EPS)[:, None]
    return (stream * rscale_second * gain_second).astype(bf16)


def solution(mesh):
    torus = Mesh(mesh.devices.reshape(16, 4, mesh.shape["cb"]), ("z", "y", "cb"))
    in_specs = (
        P(RA, "cb"),
        P("cb"),
        P(RA, "cb"),
        P(RA),
        P(RA, "cb"),
        P(RA),
        P(RA, "cb"),
        P("cb"),
        P("cb"),
    )
    return jax.shard_map(
        per_device, mesh=torus, in_specs=in_specs, out_specs=P(RA, "cb"), check_vma=False
    )
```

```python
import jax
import jax.numpy as jnp
from jax import lax
from jax.experimental import pallas as pl
from jax.experimental.pallas import tpu as pltpu
from jax.sharding import Mesh
from jax.sharding import PartitionSpec as P


RA = ("z", "y")
EPS = 1e-06
GATHER = [[*range(10, 16), *range(10)]]
SUM = [[*range(10, 16), *range(10)]]
FIRST = [(0, 1), (1, 0), (2, 3), (3, 2)]
SECOND = [(1, 2), (2, 1), (3, 0), (0, 3)]
NEAR = [[*range(5, 8), *range(5)]]
LANES = 128
USED = 352
DOWN = 368
WIDE = 384
SPLIT = 240


def whole(value):
    shape = value.shape
    return pl.BlockSpec(shape, lambda _: (0,) * len(shape))


def local(kernel, out, args, specs=None, scratch=(), flops=10**6):
    return pl.pallas_call(
        kernel,
        grid=(1,),
        in_specs=specs or [whole(arg) for arg in args],
        out_specs=whole(out),
        out_shape=out,
        scratch_shapes=scratch,
        compiler_params=pltpu.CompilerParams(vmem_limit_bytes=16 * 2**20),
        cost_estimate=pl.CostEstimate(
            flops=flops,
            bytes_accessed=sum(arg.size * arg.dtype.itemsize for arg in (*args, out)),
            transcendentals=0,
        ),
    )(*args)


def pack_kernel(
    gate_hbm,
    up_hbm,
    down_hbm,
    gate_scale_hbm,
    up_scale_hbm,
    gain_first_hbm,
    gain_second_hbm,
    down_scale_hbm,
    rows_hbm,
    out_ref,
    gain_first_ref,
    gain_second_ref,
    down_scale_ref,
    rows_ref,
    sent_hbm,
    gate_ref,
    up_ref,
    down_ref,
    gate_scale_ref,
    up_scale_ref,
    end_ref,
    block_ref,
    sems,
):
    bf16, f32 = jnp.bfloat16, jnp.float32
    units = gate_ref.shape[0]
    rest = units - LANES
    pairs = (
        (rows_hbm, rows_ref),
        (gate_hbm, gate_ref),
        (up_hbm, up_ref),
        (gate_scale_hbm, gate_scale_ref),
        (up_scale_hbm, up_scale_ref),
        (down_hbm, down_ref),
        (gain_first_hbm, gain_first_ref),
        (gain_second_hbm, gain_second_ref),
        (down_scale_hbm, down_scale_ref),
    )
    copies = [
        pltpu.make_async_copy(source, target, sems.at[place])
        for place, (source, target) in enumerate(pairs)
    ]
    for copy in copies:
        copy.start()
    end_ref[...] = jnp.zeros_like(end_ref)

    second = 2 * LANES
    third = second + rest
    fourth = third + rest
    copies[0].wait()
    rows = rows_ref[...].astype(f32)
    blocks, size, _ = block_ref.shape
    for block in range(blocks):
        block_ref[block] = rows[block * size : (block + 1) * size].astype(bf16)
    sends = [
        pltpu.make_async_copy(block_ref, sent_hbm.at[peer], sems.at[len(copies) + peer])
        for peer in range(sent_hbm.shape[0])
    ]
    for send in sends:
        send.start()
    copies[1].wait()
    out_ref[0:LANES] = gate_ref[0:LANES].astype(bf16)
    out_ref[second:third] = gate_ref[LANES:units].astype(bf16)
    copies[2].wait()
    out_ref[LANES:second] = up_ref[0:LANES].astype(bf16)
    out_ref[third:fourth] = up_ref[LANES:units].astype(bf16)

    copies[3].wait()
    copies[4].wait()
    end_ref[0:1, 0:rest] = gate_scale_ref[0:1, LANES:units]
    end_ref[8:9, 0:rest] = up_scale_ref[0:1, LANES:units]
    ends = end_ref[0:8] + pltpu.roll(end_ref[8:16], rest, 1)
    tiles = (gate_scale_ref[0:1, 0:LANES], up_scale_ref[0:1, 0:LANES], ends[0:1])
    row = lax.broadcasted_iota(jnp.int32, (DOWN - fourth, LANES), 0)
    for place, value in enumerate(tiles):
        high = value.astype(bf16).astype(f32)
        left = value - high
        middle = left.astype(bf16).astype(f32)
        low = left - middle
        pad = jnp.where(row == 0, high, 0.0)
        pad = jnp.where(row == 1, middle, pad)
        pad = jnp.where(row == 2, low, pad)
        out_ref[fourth:DOWN, place * LANES : (place + 1) * LANES] = pad.astype(bf16)
    out_ref[fourth:DOWN, 3 * LANES :] = jnp.zeros(
        (DOWN - fourth, out_ref.shape[1] - 3 * LANES), bf16
    )
    copies[5].wait()
    out_ref[DOWN : DOWN + units] = down_ref[...].astype(bf16)
    for copy in copies[6:] + sends:
        copy.wait()


def part_kernel(
    token_ref,
    gain_ref,
    own_ref,
    before_ref,
    after_ref,
    upper_ref,
    lower_ref,
    out_ref,
    far_ref,
):
    bf16, f32 = jnp.bfloat16, jnp.float32
    wide = token_ref[...].astype(f32)
    squares = jnp.sum(wide * wide, axis=1, keepdims=True)
    high = squares.astype(bf16).astype(f32)
    low = squares - high
    scaled = (wide * gain_ref[...]).astype(bf16)

    def product(rows):
        return lax.dot_general(
            scaled, rows, (((1,), (1,)), ((), ())), preferred_element_type=f32
        )

    far_ref[0:SPLIT] = upper_ref[...]
    far_ref[SPLIT:WIDE] = lower_ref[0 : WIDE - SPLIT]
    first = product(own_ref[0:WIDE])
    place = lax.broadcasted_iota(jnp.int32, first.shape, 1)
    first = jnp.where(place == USED, high, first)
    first = jnp.where(place == USED + 1, low, first)
    out_ref[:, 0:WIDE] = first.astype(bf16)
    out_ref[:, WIDE : 2 * WIDE] = product(before_ref[0:WIDE]).astype(bf16)
    out_ref[:, 2 * WIDE : 3 * WIDE] = product(after_ref[0:WIDE]).astype(bf16)
    out_ref[:, 3 * WIDE : 4 * WIDE] = product(far_ref[...]).astype(bf16)


def hidden_kernel(
    features, rest, part_ref, own_ref, before_ref, after_ref, lower_ref, out_ref
):
    bf16, f32 = jnp.bfloat16, jnp.float32
    peers, _, _ = out_ref.shape

    def summed(first):
        total = part_ref[0, :, first : first + LANES].astype(f32)
        for peer in range(1, peers):
            total = total + part_ref[peer, :, first : first + LANES].astype(f32)
        return total

    mixed = summed(2 * LANES)
    place = lax.broadcasted_iota(jnp.int32, mixed.shape, 1)
    mark = USED - 2 * LANES
    squares = jnp.where((place == mark) | (place == mark + 1), mixed, 0.0)
    squares = jnp.sum(squares, axis=1, keepdims=True)
    rscale = lax.rsqrt(squares / features + EPS)

    def store(first, value):
        for peer in range(peers):
            out_ref[peer, :, first : first + LANES] = value.astype(bf16)

    def gated(gate, up):
        return gate / (1.0 + jnp.exp(-gate)) * up

    ends = []
    for index, ref in enumerate((own_ref, before_ref, after_ref, lower_ref)):
        scales = ref[...].astype(f32)
        scales = scales[0:1] + scales[1:2] + scales[2:3]
        first = index * WIDE
        gate = summed(first) * rscale * scales[:, 0:LANES]
        up = summed(first + LANES) * rscale * scales[:, LANES : 2 * LANES]
        store(index * LANES, gated(gate, up))
        end = mixed if index == 0 else summed(first + 2 * LANES)
        end = end * rscale * scales[:, 2 * LANES : 3 * LANES]
        end = gated(end, pltpu.roll(end, LANES - rest, 1))
        ends.append(jnp.where(place < rest, end, 0.0))
    for pair in range(2):
        joined = ends[2 * pair] + pltpu.roll(ends[2 * pair + 1], LANES // 2, 1)
        store((4 + pair) * LANES, joined)


def down_kernel(
    rest, hidden_ref, own_ref, before_ref, after_ref, lower_ref, out_ref, ends_ref
):
    f32 = jnp.float32
    total = None
    ends_ref[...] = jnp.zeros_like(ends_ref)
    for index, ref in enumerate((own_ref, before_ref, after_ref, lower_ref)):
        first = DOWN - SPLIT if index == 3 else DOWN
        value = jnp.dot(
            hidden_ref[:, index * LANES : (index + 1) * LANES],
            ref[first : first + LANES],
            preferred_element_type=f32,
        )
        total = value if total is None else total + value
        start = index * (LANES // 2)
        ends_ref[start : start + rest] = ref[first + LANES : first + LANES + rest]
    total = total + jnp.dot(
        hidden_ref[:, 4 * LANES : 6 * LANES], ends_ref[...], preferred_element_type=f32
    )
    out_ref[...] = total.astype(out_ref.dtype)


def per_device(
    activations,
    gain_first,
    gate_weight,
    gate_scale,
    up_weight,
    up_scale,
    down_weight,
    down_scale,
    gain_second,
):
    bf16, f32 = jnp.bfloat16, jnp.float32
    units, width = gate_weight.shape
    rest = units - LANES
    peers = lax.axis_size("cb")
    features = width * peers
    shape = jax.ShapeDtypeStruct

    weight, scale, vector = (units, width), (1, units), pltpu.VMEM((1, width), f32)
    columns = lax.axis_size("z")
    block = (activations.shape[0] // 4, 4, width)
    sent = shape((columns, *block), bf16)
    own = pltpu.VMEM((DOWN + units, width), bf16)
    rows = pltpu.VMEM(activations.shape, bf16)
    outs = (own, vector, vector, vector, rows, sent)
    own, gain_first, gain_second, down_scale, rows, sent = pl.pallas_call(
        pack_kernel,
        in_specs=[pl.BlockSpec(memory_space=pltpu.MemorySpace.HBM)] * 9,
        out_specs=[pl.BlockSpec(memory_space=pltpu.MemorySpace.VMEM)] * 5
        + [pl.BlockSpec(memory_space=pltpu.MemorySpace.HBM)],
        out_shape=outs,
        scratch_shapes=[
            *[pltpu.VMEM(weight, f32)] * 3,
            *[pltpu.VMEM(scale, f32)] * 2,
            pltpu.VMEM((16, LANES), f32),
            pltpu.VMEM(block, bf16),
            pltpu.SemaphoreType.DMA((9 + columns,)),
        ],
        compiler_params=pltpu.CompilerParams(vmem_limit_bytes=65000000),
        cost_estimate=pl.CostEstimate(
            flops=10**6, bytes_accessed=2**20, transcendentals=0
        ),
    )(
        gate_weight,
        up_weight,
        down_weight,
        gate_scale[None],
        up_scale[None],
        gain_first[None],
        gain_second[None],
        down_scale[None],
        activations,
    )
    before = lax.ppermute(own, "y", FIRST)
    after = lax.ppermute(own, "y", SECOND)
    lower = lax.ppermute(before[SPLIT:], "y", SECOND)
    upper = lax.ppermute(after[:SPLIT], "y", FIRST)

    tokens = lax.all_to_all(sent, "z", 0, 0, tiled=True, axis_index_groups=GATHER)
    tokens = tokens.reshape(-1, width)
    count = tokens.shape[0]
    part = local(
        part_kernel,
        shape((count, 4 * WIDE), bf16),
        (tokens, gain_first, own, before, after, upper, lower),
        scratch=[pltpu.VMEM((WIDE, width), bf16)],
        flops=2 * count * width * 4 * WIDE,
    )
    part = part.reshape(peers, -1, 4 * WIDE)
    part = lax.all_to_all(part, "cb", 0, 0, tiled=True, axis_index_groups=NEAR)

    def scale_rows(first):
        return pl.BlockSpec((16, width), lambda _: (first // 16, 0))

    args = (part, own, before, after, lower)
    hidden = local(
        lambda *refs: hidden_kernel(features, rest, *refs),
        shape((peers, count // peers, 6 * LANES), bf16),
        args,
        specs=[whole(part)]
        + [scale_rows(2 * units)] * 3
        + [scale_rows(2 * units - SPLIT)],
    )
    hidden = lax.all_to_all(hidden, "cb", 0, 0, tiled=True, axis_index_groups=NEAR)
    hidden = hidden.reshape(count, 6 * LANES)
    mixed = local(
        lambda *refs: down_kernel(rest, *refs),
        shape((count, width), bf16),
        (hidden, own, before, after, lower),
        scratch=[pltpu.VMEM((2 * LANES, width), bf16)],
        flops=2 * count * width * 6 * LANES,
    )
    blocks = mixed.reshape(columns, -1, 4, width)
    summed = lax.all_to_all(blocks, "z", 0, 0, tiled=True, axis_index_groups=SUM)
    summed = jnp.sum(summed.astype(f32), axis=0).reshape(-1, width)
    stream = 0.1 * rows.astype(f32) + summed * down_scale
    second = jnp.sum(stream * stream, axis=1)
    second = jnp.broadcast_to(second, (peers, *second.shape))
    second = lax.all_to_all(second, "cb", 0, 0, tiled=True, axis_index_groups=NEAR)
    second = jnp.sum(second, axis=0)
    rscale_second = lax.rsqrt(second / features + EPS)[:, None]
    return (stream * rscale_second * gain_second).astype(bf16)


def solution(mesh):
    torus = Mesh(mesh.devices.reshape(16, 4, mesh.shape["cb"]), ("z", "y", "cb"))
    in_specs = (
        P(RA, "cb"),
        P("cb"),
        P(RA, "cb"),
        P(RA),
        P(RA, "cb"),
        P(RA),
        P(RA, "cb"),
        P("cb"),
        P("cb"),
    )
    return jax.shard_map(
        per_device, mesh=torus, in_specs=in_specs, out_specs=P(RA, "cb"), check_vma=False
    )
```
